256 devices in a mesh: grp: 2 (over y), ep: 64 (over z, x), tp: 2 (over core).
Axes of the slice: x: 4, y: 2, z: 16, core: 2. Of those that a mesh axis runs over, the one named last changes fastest.
The devices are a block of a 4x16x16 slice.
Arguments:
- tokens: bfloat16 [4096, 1024], P(('grp', 'ep', 'tp')), parts along dimension 0, may hold values from -1.75 to 1.75
- latent_cache: bfloat16 [4096, 1024, 256], P(('grp', 'ep', 'tp')), parts along dimension 0, may hold values from -6 to 6
- rope_cache: bfloat16 [4096, 1024, 32], P(('grp', 'ep', 'tp')), parts along dimension 0, may hold values from -1200 to 1200
- lengths: int32 [4096], P(('grp', 'ep', 'tp')), parts along dimension 0, may hold values from 128 to 1024
- expert_ids: int32 [4096, 4], P(('grp', 'ep', 'tp')), parts along dimension 0, may hold values from 0 to 127, all different within a row; in each aligned block of 16 rows (0 to 15, 16 to 31, ...) at most 4 rows name the same one
- route_weights: float32 [4096, 4], P(('grp', 'ep', 'tp')), parts along dimension 0, may hold values from 0.1 to 1
- g_attn: float32 [1024], replicated, may hold values from 0.1 to 1.9
- w_query_down: bfloat16 [1024, 256], replicated, may hold values from -0.1875 to 0.1875
- g_query: float32 [256], replicated, may hold values from 0.1 to 1.9
- w_latent_down: bfloat16 [1024, 256], replicated, may hold values from -0.1875 to 0.1875
- g_latent: float32 [256], replicated, may hold values from 0.1 to 1.9
- w_rope_key: bfloat16 [1024, 32], replicated, may hold values from -0.1875 to 0.1875
- w_query: bfloat16 [256, 1024], replicated, may hold values from -0.375 to 0.375
- w_query_rope: bfloat16 [256, 512], replicated, may hold values from -0.375 to 0.375
- w_key_up: bfloat16 [256, 1024], replicated, may hold values from -0.875 to 0.875
- w_value_up: bfloat16 [256, 1024], replicated, may hold values from -0.375 to 0.375
- w_out: bfloat16 [1024, 1024], replicated, may hold values from -0.1875 to 0.1875
- g_ffn: float32 [1024], replicated, may hold values from 0.1 to 1.9
- w_expert_gate: bfloat16 [128, 1024, 256], P('ep', None, 'tp'), may hold values from -0.1875 to 0.1875
- w_expert_up: bfloat16 [128, 1024, 256], P('ep', None, 'tp'), may hold values from -0.1875 to 0.1875
- w_expert_down: bfloat16 [128, 256, 1024], P('ep', 'tp'), may hold values from -0.375 to 0.375
- w_shared_gate: bfloat16 [1024, 256], replicated, may hold values from -0.1875 to 0.1875
- w_shared_up: bfloat16 [1024, 256], replicated, may hold values from -0.1875 to 0.1875
- w_shared_down: bfloat16 [256, 1024], replicated, may hold values from -0.375 to 0.375
Outputs:
- mixed_out: bfloat16 [4096, 1024], P(('grp', 'ep', 'tp')), parts along dimension 0
- new_entry: bfloat16 [4096, 288], P(('grp', 'ep', 'tp')), parts along dimension 0
The draws below stay inside these ranges and needn't reach their ends.
There are 2 independent parts, one for each index of `grp`. The reference program is written for one: setup_inputs(seed, part) draws one part's arguments, and reference() takes and returns one part's arrays. A program takes and returns all parts, laid end to end along the dimension named above; an argument that names none is the same for every part. Nothing has to cross between parts.
Inputs may be any that keep to these rules, and one draw needn't show every extreme that they name: `expert_ids`: each row names 4 different experts. In the aligned blocks of rows that one device holds (one block for each device of ep and tp together), no expert is named by more than 4 rows, a bound that some block reaches.
All inputs are finite; a program needn't handle non-finite values.
Results may differ from the reference program's by a relative error of at most 0.03.
Values may be sent and summed in bfloat16 or wider, within the bound.
A program may use at most 64 MiB of HBM per device.

```python
import math
import jax
import jax.numpy as jnp
import numpy as np
from jax import lax

D = 1024
HEADS = 16
QLORA = 256
KVLORA = 256
NOPE = 64
ROPE = 32
VDIM = 64
EFF = 256
SFF = 256
TOPK = 4
SEQS = 32
CACHE_LEN = 1024
EXPERTS = 128
CAP = 4
BATCH = 2048
N_EP = 64
N_TP = 2


def draw_rope_cache(key, part):
    base_draw = jax.random.truncated_normal(key, -4.0, 4.0, (BATCH, CACHE_LEN, ROPE), jnp.float32)
    return base_draw.astype(jnp.bfloat16)


def plant(result, stream_key, least, largest):
    longest = result.shape.index(max(result.shape))
    spots = []
    for shift in (0, 1):
        where = [jax.random.randint(jax.random.fold_in(stream_key, axis), (), 0, length) for axis, length in enumerate(result.shape)]
        where[longest] = (where[longest] + shift) % result.shape[longest]
        spots.append(tuple(where))
    return result.at[spots[0]].set(least).at[spots[1]].set(largest)


def level_of(stream_key, shape, pieces, low, high):
    factor_of = 1.0
    for position, blocks in pieces:
        draws = jax.random.uniform(jax.random.fold_in(jax.random.fold_in(stream_key, 6), position), (blocks,), jnp.float32, low / len(pieces), high / len(pieces))
        factor_of = factor_of * jnp.repeat(jnp.exp(draws), shape[position] // blocks).reshape((-1,) + (1,) * (len(shape) - 1 - position))
    return factor_of


def routed_block(rng, own, number, rows, count, top, limit, slope):
    ranking = jax.random.permutation(rng, count)
    crowded, common = portions_of(count, rows * top, limit, slope, True), portions_of(count, rows * top, limit, slope, False)
    places = jnp.arange(count)

    def named(sizes, rotation):
        used = int((sizes > 0).sum())
        fixed = max(1, used // 4)
        shifted = fixed + (places - fixed + rotation * (used - fixed)) % max(1, count - fixed)
        return jnp.zeros((count,), jnp.int32).at[ranking[jnp.where(places < fixed, places, shifted)]].set(jnp.asarray(sizes, jnp.int32))

    sizes = jnp.where(number % 4 == 0, named(crowded, number // 4), named(common, number - number // 4 - 1))
    mixed = jax.random.permutation(jax.random.fold_in(own, 3), count)
    donor, taker = mixed[0:count // 2 * 2:2], mixed[1:count // 2 * 2:2]
    room = jnp.minimum(sizes[donor] - 1, limit - sizes[taker]) // 2
    room = jnp.where((donor == ranking[0]) | (taker == ranking[0]) | (sizes[taker] == 0), 0, jnp.maximum(room, 0))
    shifted = jax.random.randint(jax.random.fold_in(own, 4), (count // 2,), 0, 1 << 20) % (room + 1)
    sizes = sizes.at[donor].add(-shifted).at[taker].add(shifted)
    members = jnp.searchsorted(jnp.cumsum(sizes), jnp.arange(rows * top), side="right").astype(jnp.int32)
    listing = members.reshape(top, rows).T
    listing = listing[jax.random.permutation(jax.random.fold_in(own, 1), rows)]
    rotation = jax.random.randint(jax.random.fold_in(own, 2), (rows, 1), 0, top)
    return jnp.take_along_axis(listing, (jnp.arange(top)[None, :] + rotation) % top, axis=1)


def portions_of(number_of, total, reach, lean, full):
    portions = [(1 << 20) // math.isqrt(standing ** lean) + 1 for standing in range(1, number_of + 1)]
    largest = reach if full else min(reach, max(-(-total // number_of), total * portions[0] // sum(portions)))
    least = 1 if total - largest >= number_of - 1 else 0
    counts, surplus = [largest] + [least] * (number_of - 1), total - largest - least * (number_of - 1)
    while surplus > 0:
        free = [i for i in range(1, number_of) if counts[i] < largest] or [i for i in range(1, number_of) if counts[i] < reach]
        pool, budget = sum([portions[i] for i in free]), surplus
        for i in free:
            more = min(reach - counts[i], max(1, budget * portions[i] // pool), surplus)
            counts[i] = counts[i] + more
            surplus = surplus - more
    return np.array(counts)


def noise(stream_key, shape, scale, reach, pieces=(), kind=jnp.bfloat16):
    values = jax.random.normal(stream_key, shape, jnp.float32) * scale
    if len(pieces) > 0:
        values = level_of(stream_key, shape, pieces, -0.22, 0.18) * values
    return jnp.clip(values, min=-reach, max=reach).astype(kind)


def setup_inputs(seed: int = 0, part: int = 0) -> dict:
    seeds = jax.random.split(jax.random.key(seed), 25)
    part_keys = jax.random.split(jax.random.fold_in(seeds[24], part), 25)
    tokens = noise(part_keys[0], (BATCH, D), 0.3, 1.75, ((0, 128),))
    latent_cache = noise(part_keys[1], (BATCH, CACHE_LEN, KVLORA), 1.0, 6.0, ((0, 128),))
    rope_cache = draw_rope_cache(jax.random.fold_in(jax.random.fold_in(seeds[24], part), 71), part)
    lengths = plant(jax.random.randint(part_keys[3], (BATCH,), CACHE_LEN // 8, CACHE_LEN + 1), jax.random.fold_in(part_keys[3], 1), CACHE_LEN // 8, CACHE_LEN).astype(jnp.int32)
    expert_ids_keys = jax.random.split(jax.random.fold_in(part_keys[4], 1), BATCH // (SEQS // N_TP))
    expert_ids_turns = jax.random.permutation(jax.random.fold_in(part_keys[4], 3), BATCH // (SEQS // N_TP))
    expert_ids = jax.vmap(lambda own, number: routed_block(jax.random.fold_in(part_keys[4], 2), own, number, SEQS // N_TP, EXPERTS, TOPK, CAP, 2))(expert_ids_keys, expert_ids_turns).reshape((BATCH, TOPK))
    route_weights = jnp.clip(jnp.exp(math.log(1.0) - 2.3025851 * jax.random.uniform(part_keys[5], (BATCH, TOPK), jnp.float32) ** level_of(part_keys[5], (BATCH, TOPK), ((0, 128),), -0.2, 0.2)), 0.1, 1.0)
    g_attn = jnp.clip(1.0 + 0.18 * jax.random.normal(seeds[6], (D,), jnp.float32), 0.1, 1.9)
    w_query_down = noise(seeds[7], (D, QLORA), D ** -0.5, 0.1875)
    g_query = jnp.clip(1.0 + 0.18 * jax.random.normal(seeds[8], (QLORA,), jnp.float32), 0.1, 1.9)
    w_latent_down = noise(seeds[9], (D, KVLORA), D ** -0.5, 0.1875)
    g_latent = jnp.clip(1.0 + 0.18 * jax.random.normal(seeds[10], (KVLORA,), jnp.float32), 0.1, 1.9)
    w_rope_key = noise(seeds[11], (D, ROPE), D ** -0.5, 0.1875)
    w_query = noise(seeds[12], (QLORA, HEADS * NOPE), QLORA ** -0.5, 0.375)
    w_query_rope = noise(seeds[13], (QLORA, HEADS * ROPE), QLORA ** -0.5, 0.375)
    w_key_up = noise(seeds[14], (KVLORA, HEADS * NOPE), 0.15, 0.875)
    w_value_up = noise(seeds[15], (KVLORA, HEADS * VDIM), KVLORA ** -0.5, 0.375)
    w_out = noise(seeds[16], (HEADS * VDIM, D), (HEADS * VDIM) ** -0.5, 0.1875)
    g_ffn = jnp.clip(1.0 + 0.18 * jax.random.normal(seeds[17], (D,), jnp.float32), 0.1, 1.9)
    w_expert_gate = noise(seeds[18], (EXPERTS, D, EFF), D ** -0.5, 0.1875, ((0, 64), (2, 2)))
    w_expert_up = noise(seeds[19], (EXPERTS, D, EFF), D ** -0.5, 0.1875, ((0, 64), (2, 2)))
    w_expert_down = noise(seeds[20], (EXPERTS, EFF, D), EFF ** -0.5, 0.375, ((0, 64), (1, 2)))
    w_shared_gate = noise(seeds[21], (D, SFF), D ** -0.5, 0.1875)
    w_shared_up = noise(seeds[22], (D, SFF), D ** -0.5, 0.1875)
    w_shared_down = noise(seeds[23], (SFF, D), SFF ** -0.5, 0.375)
    return {"tokens": tokens, "latent_cache": latent_cache, "rope_cache": rope_cache, "lengths": lengths, "expert_ids": expert_ids, "route_weights": route_weights, "g_attn": g_attn, "w_query_down": w_query_down, "g_query": g_query, "w_latent_down": w_latent_down, "g_latent": g_latent, "w_rope_key": w_rope_key, "w_query": w_query, "w_query_rope": w_query_rope, "w_key_up": w_key_up, "w_value_up": w_value_up, "w_out": w_out, "g_ffn": g_ffn, "w_expert_gate": w_expert_gate, "w_expert_up": w_expert_up, "w_expert_down": w_expert_down, "w_shared_gate": w_shared_gate, "w_shared_up": w_shared_up, "w_shared_down": w_shared_down}


norm_eps = 1e-06
rope_theta = 10000.0
masked_score = -1e+30

def rms_scale(values, gain_vec):
    mean_square = lax.optimization_barrier(jnp.mean(values * values, axis=-1, keepdims=True))
    return values * lax.rsqrt(mean_square + norm_eps) * gain_vec.astype(jnp.float32)

def rotate(values, positions):
    half_width = values.shape[-1] // 2
    frequency = rope_theta ** (-jnp.arange(half_width, dtype=jnp.float32) / half_width)
    angles = positions.astype(jnp.float32)[:, None] * frequency[None, :]
    angles = angles.reshape(angles.shape[:1] + (1,) * (values.ndim - 2) + (half_width,))
    cosine = jnp.cos(angles)
    sine_part = jnp.sin(angles)
    first_half = values[..., :half_width]
    second_half = values[..., half_width:]
    return jnp.concatenate([first_half * cosine - second_half * sine_part, first_half * sine_part + second_half * cosine], axis=-1)

def attend_block(block_args):
    query_latent, query_rope, cache_latent, cache_rope, length = block_args
    scores = (jnp.einsum('shc,stc->sht', query_latent.astype(jnp.float32), cache_latent.astype(jnp.float32)) + jnp.einsum('shr,str->sht', query_rope.astype(jnp.float32), cache_rope.astype(jnp.float32))) * (NOPE + ROPE) ** (-0.5)
    live_mask = jnp.arange(CACHE_LEN, dtype=jnp.int32)[None, None, :] < length[:, None, None]
    row_max = lax.optimization_barrier(jnp.max(jnp.where(live_mask, scores, masked_score), axis=2, keepdims=True))
    weights = jnp.where(live_mask, jnp.exp(scores - row_max), 0.0)
    weight_sum = lax.optimization_barrier(jnp.sum(weights, axis=2))
    rounded = lax.optimization_barrier(weights.astype(jnp.bfloat16)).astype(jnp.float32)
    mixed_latent = jnp.einsum('sht,stc->shc', rounded, cache_latent.astype(jnp.float32))
    return (mixed_latent / weight_sum[:, :, None]).astype(jnp.bfloat16)

def reference(tokens, latent_cache, rope_cache, lengths, expert_ids, route_weights, g_attn, w_query_down, g_query, w_latent_down, g_latent, w_rope_key, w_query, w_query_rope, w_key_up, w_value_up, w_out, g_ffn, w_expert_gate, w_expert_up, w_expert_down, w_shared_gate, w_shared_up, w_shared_down):
    row_count = tokens.shape[0]
    normed = rms_scale(tokens.astype(jnp.float32), g_attn).astype(jnp.bfloat16)
    query_low = rms_scale(jnp.dot(normed, w_query_down, preferred_element_type=jnp.float32), g_query).astype(jnp.bfloat16)
    latent_new = rms_scale(jnp.dot(normed, w_latent_down, preferred_element_type=jnp.float32), g_latent).astype(jnp.bfloat16)
    key_new = rotate(jnp.dot(normed, w_rope_key, preferred_element_type=jnp.float32), lengths).astype(jnp.bfloat16)
    new_entry = jnp.concatenate([latent_new, key_new], axis=1)
    query_nope = jnp.dot(query_low, w_query, preferred_element_type=jnp.float32).astype(jnp.bfloat16)
    query_nope = query_nope.reshape(row_count, HEADS, NOPE)
    query_turn = jnp.dot(query_low, w_query_rope, preferred_element_type=jnp.float32).reshape(row_count, HEADS, ROPE)
    query_rope = rotate(query_turn, lengths).astype(jnp.bfloat16)
    query_latent = jnp.einsum('bhn,chn->bhc', query_nope.astype(jnp.float32), w_key_up.reshape(KVLORA, HEADS, NOPE).astype(jnp.float32)).astype(jnp.bfloat16)
    block_size = SEQS // N_TP
    block_count = row_count // block_size
    latent_mix = lax.map(attend_block, (query_latent.reshape(block_count, block_size, HEADS, KVLORA), query_rope.reshape(block_count, block_size, HEADS, ROPE), latent_cache.reshape(block_count, block_size, CACHE_LEN, KVLORA), rope_cache.reshape(block_count, block_size, CACHE_LEN, ROPE), lengths.reshape(block_count, block_size))).reshape(row_count, HEADS, KVLORA)
    value_heads = jnp.einsum('bhc,chv->bhv', latent_mix.astype(jnp.float32), w_value_up.reshape(KVLORA, HEADS, VDIM).astype(jnp.float32)).astype(jnp.bfloat16)
    attn_out = jnp.dot(value_heads.reshape(row_count, HEADS * VDIM), w_out, preferred_element_type=jnp.float32)
    hidden_state = (tokens.astype(jnp.float32) + attn_out).astype(jnp.bfloat16)
    normed_ffn = rms_scale(hidden_state.astype(jnp.float32), g_ffn).astype(jnp.bfloat16)
    shared_gate = jnp.dot(normed_ffn, w_shared_gate, preferred_element_type=jnp.float32)
    shared_up = jnp.dot(normed_ffn, w_shared_up, preferred_element_type=jnp.float32)
    shared_hidden = (jax.nn.silu(shared_gate) * shared_up).astype(jnp.bfloat16)
    shared_out = jnp.dot(shared_hidden, w_shared_down, preferred_element_type=jnp.float32)
    expert_count = w_expert_gate.shape[0]
    most_rows = N_EP * N_TP * CAP
    half_width = EFF // N_TP
    padded = jnp.concatenate([normed_ffn, jnp.zeros((1, D), jnp.bfloat16)], axis=0)

    def per_expert(routed_sum, expert):
        names_it = expert_ids == expert
        weight = lax.optimization_barrier(jnp.sum(jnp.where(names_it, route_weights, 0.0), axis=1))
        weight_pad = jnp.concatenate([weight, jnp.zeros((1,), jnp.float32)])
        picked = jnp.nonzero(jnp.any(names_it, axis=1), size=most_rows, fill_value=row_count)[0].astype(jnp.int32)
        inputs = padded[picked]
        gate_value = jnp.dot(inputs, w_expert_gate[expert], preferred_element_type=jnp.float32)
        up_value = jnp.dot(inputs, w_expert_up[expert], preferred_element_type=jnp.float32)
        hidden = (jax.nn.silu(gate_value) * up_value).astype(jnp.bfloat16)
        part_total = jnp.zeros((most_rows, D), jnp.float32)
        for part_index in range(N_TP):
            part_piece = jnp.dot(hidden[:, part_index * half_width:(part_index + 1) * half_width], w_expert_down[expert, part_index * half_width:(part_index + 1) * half_width], preferred_element_type=jnp.float32)
            part_total = part_total + lax.optimization_barrier(part_piece.astype(jnp.bfloat16)).astype(jnp.float32)
        expert_out = lax.optimization_barrier(part_total.astype(jnp.bfloat16)).astype(jnp.float32)
        routed_sum = routed_sum.at[picked].add(weight_pad[picked][:, None] * expert_out)
        return (routed_sum, None)
    routed, _ = lax.scan(per_expert, jnp.zeros((row_count + 1, D), jnp.float32), jnp.arange(expert_count, dtype=jnp.int32))
    mixed_out = (hidden_state.astype(jnp.float32) + routed[:row_count] + shared_out).astype(jnp.bfloat16)
    return (mixed_out, new_entry)
```

```python
import functools

import jax
import jax.numpy as jnp
from jax import lax
from jax.experimental import pallas as pl
from jax.experimental.pallas import tpu as pltpu
from jax.sharding import PartitionSpec as P

D = 1024
HEADS = 16
KVLORA = 256
NOPE = 64
ROPE = 32
VDIM = 64


norm_eps = 1e-06
rope_theta = 10000.0
masked_score = -1e30


def rms_scale(values, gain_vec):
    mean_square = jnp.mean(values * values, axis=-1, keepdims=True)
    return values * lax.rsqrt(mean_square + norm_eps) * gain_vec


def rotate(values, positions):
    half_width = values.shape[-1] // 2
    frequency = rope_theta ** (-jnp.arange(half_width, dtype=jnp.float32) / half_width)
    angles = positions.astype(jnp.float32)[:, None] * frequency[None, :]
    angles = angles.reshape(angles.shape[:1] + (1,) * (values.ndim - 2) + (half_width,))
    cosine = jnp.cos(angles)
    sine_part = jnp.sin(angles)
    first_half = values[..., :half_width]
    second_half = values[..., half_width:]
    return jnp.concatenate(
        [
            first_half * cosine - second_half * sine_part,
            first_half * sine_part + second_half * cosine,
        ],
        axis=-1,
    )


MESH = pl.DeviceIdType.MESH
RING_X = 4
EFF2 = 256
HALF = 128


def remote(src, dst, send_sem, recv_sem, **where):
    return pltpu.make_async_remote_copy(
        src_ref=src,
        dst_ref=dst,
        send_sem=send_sem,
        recv_sem=recv_sem,
        device_id=where,
        device_id_type=MESH,
    )


def moe_kernel(
    ep_size,
    x_ref,
    meta_ref,
    base_ref,
    gate_hbm,
    up_hbm,
    down_hbm,
    out_ref,
    rows_buf,
    part_buf,
    meta_buf,
    w_in,
    w_down,
    half_l,
    half_r,
    full_l,
    full_r,
    chain_a,
    chain_b,
    w_local,
    w_send,
    w_recv,
    m_send,
    m_recv,
    zs,
    zr,
    xs,
    xr,
    rs_xs,
    rs_xr,
    rs_zs,
    rs_zr,
):
    ring_z = ep_size // RING_X
    far = ring_z // 2
    me = lax.axis_index("ep")
    core = lax.axis_index("tp")
    z = me // RING_X
    x = me % RING_X
    low, high = pl.ds(0, D // 2), pl.ds(D // 2, D // 2)

    def at(zz, xx):
        return lax.rem(zz + 2 * ring_z, ring_z) * RING_X + lax.rem(xx + 2 * RING_X, RING_X)

    right, left = at(z, x + 1), at(z, x - 1)
    above, below = at(z + 1, x), at(z - 1, x)

    barrier = pltpu.get_barrier_semaphore()

    def greet(step, carry):
        pl.semaphore_signal(
            barrier, inc=1, device_id={"ep": lax.rem(me + step, ep_size)}, device_id_type=MESH
        )
        return carry

    lax.fori_loop(1, ep_size, greet, 0)
    pl.semaphore_signal(barrier, inc=1, device_id={"tp": 1 - core}, device_id_type=MESH)

    pieces = []
    for e in range(2):
        for kind, hbm in enumerate((gate_hbm, up_hbm)):
            col = pl.multiple_of((e * 2 + kind) * EFF2 + core * HALF, HALF)
            pieces.append((hbm.at[e], w_in.at[:, pl.ds(col, HALF)]))
        row = pl.multiple_of(e * EFF2 + core * HALF, HALF)
        pieces.append((down_hbm.at[e], w_down.at[pl.ds(row, HALF), :]))
    local_copies = [
        pltpu.make_async_copy(s, d, w_local.at[i]) for i, (s, d) in enumerate(pieces)
    ]
    for copy in local_copies:
        copy.start()
    rows_buf[me] = x_ref[...]
    meta_buf[me] = meta_ref[...]

    pl.semaphore_wait(barrier, ep_size)

    def z_up(t):
        slot = at(z - t, x)
        return remote(
            x_ref if isinstance(t, int) and t == 0 else rows_buf.at[slot],
            rows_buf.at[slot], zs.at[0, t], zr.at[0, t], ep=above,
        )

    def z_down(t):
        slot = at(z + t, x)
        return remote(
            x_ref if isinstance(t, int) and t == 0 else rows_buf.at[slot],
            rows_buf.at[slot], zs.at[1, t], zr.at[1, t], ep=below,
        )

    def x_near(p, zz):
        slot = at(zz, x)
        src = x_ref if isinstance(p, int) and p == 0 else rows_buf.at[slot]
        return (
            remote(src, rows_buf.at[slot], xs.at[0, p], xr.at[0, p], ep=right),
            remote(src, rows_buf.at[slot], xs.at[1, p], xr.at[1, p], ep=left),
        )

    def x_far(p, zz):
        from_left, from_right = at(zz, x - 1), at(zz, x + 1)
        return (
            remote(
                rows_buf.at[from_left, :, low], rows_buf.at[from_left, :, low],
                xs.at[2, p], xr.at[2, p], ep=right,
            ),
            remote(
                rows_buf.at[from_right, :, high], rows_buf.at[from_right, :, high],
                xs.at[3, p], xr.at[3, p], ep=left,
            ),
        )

    def start(copies):
        for copy in copies:
            copy.start()

    def arrived(copies):
        for copy in copies:
            copy.wait_recv()

    def sent(copies):
        for copy in copies:
            copy.wait_send()

    z_up(0).start()
    z_down(0).start()
    start(x_near(0, z))

    def meta_copy(step):
        return remote(
            meta_ref, meta_buf.at[me], m_send, m_recv, ep=lax.rem(me + step, ep_size)
        )

    def meta_go(step, carry):
        meta_copy(step).start()
        return carry

    lax.fori_loop(1, ep_size, meta_go, 0)

    remote_copies = [
        remote(s, d, w_send.at[i], w_recv.at[i], tp=1 - core) for i, (s, d) in enumerate(pieces)
    ]
    start(remote_copies)

    lane = lax.broadcasted_iota(jnp.int32, (16, 128), 1)
    row = lax.broadcasted_iota(jnp.int32, (16, 128), 0)
    pick = (lane < 64) & (lane % 16 == row)
    first_expert = (2 * me).astype(jnp.float32)

    def weight_columns(slot):
        ids = meta_buf[slot]
        scale = pltpu.roll(ids, 64, 1)
        columns = []
        for e in range(2):
            chosen = jnp.where(ids == first_expert + e, scale, 0.0)
            chosen = jnp.where(pick, jnp.broadcast_to(chosen, (16, 128)), 0.0)
            columns.append(jnp.sum(chosen, axis=1, keepdims=True))
        return columns

    def experts(plane_a, plane_b):
        planes = [lax.rem(plane + 2 * ring_z, ring_z) for plane in (plane_a, plane_b)]
        rows = jnp.concatenate(
            [rows_buf[pl.ds(plane * RING_X, RING_X)].reshape(RING_X * 16, D) for plane in planes], 0
        )
        scales = [weight_columns(plane * RING_X + k) for plane in planes for k in range(RING_X)]
        hidden = []
        for e in range(2):
            gates = jnp.dot(
                rows, w_in[:, 2 * e * EFF2 : (2 * e + 1) * EFF2], preferred_element_type=jnp.float32
            )
            ups = jnp.dot(
                rows, w_in[:, (2 * e + 1) * EFF2 : (2 * e + 2) * EFF2],
                preferred_element_type=jnp.float32,
            )
            scale = jnp.concatenate([s[e] for s in scales], axis=0)
            hidden.append((gates / (1.0 + jnp.exp(-gates)) * ups * scale).astype(jnp.bfloat16))
        total = jnp.dot(
            jnp.concatenate(hidden, axis=1), w_down[...], preferred_element_type=jnp.float32
        ).astype(jnp.bfloat16)
        for k, plane in enumerate(planes):
            part_buf[pl.ds(plane * RING_X, RING_X)] = total[
                k * RING_X * 16 : (k + 1) * RING_X * 16
            ].reshape(RING_X, 16, D)

    def far_of(t):
        return x_far(2 * t + 1, z - 1 - t) + x_far(2 * t + 2, z + 1 + t)

    def near_of(t):
        return x_near(2 * t + 1, z - 1 - t) + x_near(2 * t + 2, z + 1 + t)

    z_up(0).wait_recv()
    z_up(1).start()
    z_down(0).wait_recv()
    z_down(1).start()
    start(near_of(0))
    arrived(x_near(0, z))
    start(x_far(0, z))

    for copy in local_copies:
        copy.wait()
    for copy in remote_copies:
        copy.wait()
    whole_meta = meta_buf.at[pl.ds(0, ep_size - 1)]
    pltpu.make_async_copy(whole_meta, whole_meta, m_recv).wait()
    pltpu.make_async_copy(whole_meta, whole_meta, m_send).wait()

    z_up(1).wait_recv()
    z_up(2).start()
    z_down(1).wait_recv()
    z_down(2).start()
    start(near_of(1))
    arrived(near_of(0))
    start(far_of(0))
    arrived(x_far(0, z))

    def gather_step(t, carry):
        z_up(t).wait_recv()
        z_up(t + 1).start()
        z_down(t).wait_recv()

        @pl.when(t < far - 2)
        def _():
            z_down(t + 1).start()

        start(near_of(t))
        arrived(near_of(t - 1))
        start(far_of(t - 1))
        arrived(far_of(t - 2))
        experts(z - (t - 1), z + (t - 1))
        return carry

    lax.fori_loop(2, far - 1, gather_step, 0)
    last = far - 1
    z_up(last).wait_recv()
    start(x_near(2 * last + 1, z - far))
    arrived(near_of(last - 1))
    start(far_of(last - 1))
    arrived(far_of(last - 2))
    experts(z - last + 1, z + last - 1)
    arrived(x_near(2 * last + 1, z - far))
    start(x_far(2 * last + 1, z - far))
    arrived(far_of(last - 1))
    experts(z - last, z + last)
    arrived(x_far(2 * last + 1, z - far))
    experts(z, z - far)

    def plane_of(i, side):
        return z - (far - i) if side == 0 else z + (far - 1 - i)

    def x1(i):
        copies = []
        for side in range(2):
            zz, p = plane_of(i, side), 2 * i + side
            opposite = at(zz, x + 2)
            copies.append(
                remote(
                    part_buf.at[opposite, :, low], half_l.at[p],
                    rs_xs.at[0, p], rs_xr.at[0, p], ep=right,
                )
            )
            copies.append(
                remote(
                    part_buf.at[opposite, :, high], half_r.at[p],
                    rs_xs.at[1, p], rs_xr.at[1, p], ep=left,
                )
            )
        return copies

    def x2(i):
        copies = []
        for side in range(2):
            zz, p = plane_of(i, side), 2 * i + side
            copies.append(
                remote(
                    part_buf.at[at(zz, x + 1)], full_l.at[p],
                    rs_xs.at[2, p], rs_xr.at[2, p], ep=right,
                )
            )
            copies.append(
                remote(
                    part_buf.at[at(zz, x - 1)], full_r.at[p],
                    rs_xs.at[3, p], rs_xr.at[3, p], ep=left,
                )
            )
        return copies

    def x2_add(i):
        for side in range(2):
            zz, p = plane_of(i, side), 2 * i + side
            to_right, to_left = at(zz, x + 1), at(zz, x - 1)
            part_buf[to_right, :, low] = part_buf[to_right, :, low] + half_l[p]
            part_buf[to_left, :, high] = part_buf[to_left, :, high] + half_r[p]

    def chain(i, side):
        slot = at(plane_of(i, side), x)
        buf = chain_a if side == 0 else chain_b
        return remote(
            part_buf.at[slot], buf.at[i], rs_zs.at[side, i], rs_zr.at[side, i],
            ep=below if side == 0 else above,
        )

    def own_sum(i, side):
        slot, p = at(plane_of(i, side), x), 2 * i + side
        return (
            part_buf[slot].astype(jnp.float32)
            + full_l[p].astype(jnp.float32)
            + full_r[p].astype(jnp.float32)
        )

    def store(i, side, total):
        part_buf[at(plane_of(i, side), x)] = total.astype(jnp.bfloat16)

    start(x1(0))
    start(x1(1))
    arrived(x1(0))
    x2_add(0)
    start(x2(0))
    arrived(x2(0))
    for side in range(2):
        store(0, side, own_sum(0, side))
        chain(0, side).start()
    arrived(x1(1))
    x2_add(1)
    start(x2(1))
    start(x1(2))

    def sum_step(i, carry):
        arrived(x2(i))
        for side in range(2):
            total = own_sum(i, side)
            chain(i - 1, side).wait_recv()
            buf = chain_a if side == 0 else chain_b
            store(i, side, total + buf[i - 1].astype(jnp.float32))
            chain(i, side).start()
        arrived(x1(i + 1))
        x2_add(i + 1)
        start(x2(i + 1))

        @pl.when(i < far - 2)
        def _():
            start(x1(i + 2))

        return carry

    lax.fori_loop(1, far - 1, sum_step, 0)
    arrived(x2(last))
    total = own_sum(last, 0)
    chain(last - 1, 0).wait_recv()
    store(last, 0, total + chain_a[last - 1].astype(jnp.float32))
    chain(last, 0).start()
    total = own_sum(last, 1) + base_ref[...]
    chain(last - 1, 1).wait_recv()
    total = total + chain_b[last - 1].astype(jnp.float32)
    chain(last, 0).wait_recv()
    out_ref[...] = (total + chain_a[last].astype(jnp.float32)).astype(jnp.bfloat16)

    def drain_z(t, carry):
        z_up(t).wait_send()
        chain(t, 0).wait_send()

        @pl.when(t < far - 1)
        def _():
            z_down(t).wait_send()
            chain(t, 1).wait_send()

        sent(x1(t))
        sent(x2(t))
        return carry

    lax.fori_loop(0, far, drain_z, 0)

    def drain_x(p, carry):
        zz = z
        sent(x_near(p, zz))
        sent(x_far(p, zz))
        return carry

    lax.fori_loop(0, 2 * far, drain_x, 0)


def moe(rows, meta, base, w_gate, w_up, w_down):
    ep_size = lax.axis_size("ep")
    ring_z = ep_size // RING_X
    far = ring_z // 2
    count = rows.shape[0]
    bf = jnp.bfloat16
    dma = pltpu.SemaphoreType.DMA
    vm = pl.BlockSpec(memory_space=pltpu.VMEM)
    anywhere = pl.BlockSpec(memory_space=pl.ANY)
    block = (count, D)
    half = (count, D // 2)
    return pl.pallas_call(
        functools.partial(moe_kernel, ep_size),
        out_shape=jax.ShapeDtypeStruct((count, D), bf),
        in_specs=[vm, vm, vm, anywhere, anywhere, anywhere],
        out_specs=vm,
        scratch_shapes=[
            pltpu.VMEM((ep_size, *block), bf),
            pltpu.VMEM((ep_size, *block), bf),
            pltpu.VMEM((ep_size, 1, 128), jnp.float32),
            pltpu.VMEM((D, 4 * EFF2), bf),
            pltpu.VMEM((2 * EFF2, D), bf),
            pltpu.VMEM((ring_z, *half), bf),
            pltpu.VMEM((ring_z, *half), bf),
            pltpu.VMEM((ring_z, *block), bf),
            pltpu.VMEM((ring_z, *block), bf),
            pltpu.VMEM((far, *block), bf),
            pltpu.VMEM((far, *block), bf),
            dma((6,)),
            dma((6,)),
            dma((6,)),
            dma,
            dma,
            dma((2, far)),
            dma((2, far)),
            dma((4, ring_z)),
            dma((4, ring_z)),
            dma((4, ring_z)),
            dma((4, ring_z)),
            dma((2, far)),
            dma((2, far)),
        ],
        compiler_params=pltpu.CompilerParams(
            collective_id=0, has_side_effects=True, vmem_limit_bytes=40 * 1024 * 1024
        ),
        name="moe",
    )(rows, meta, base, w_gate, w_up, w_down)


def local(
    tokens,
    latent_cache,
    rope_cache,
    lengths,
    expert_ids,
    route_weights,
    g_attn,
    w_query_down,
    g_query,
    w_latent_down,
    g_latent,
    w_rope_key,
    w_query,
    w_query_rope,
    w_key_up,
    w_value_up,
    w_out,
    g_ffn,
    w_expert_gate,
    w_expert_up,
    w_expert_down,
    w_shared_gate,
    w_shared_up,
    w_shared_down,
):
    row_count = tokens.shape[0]
    normed = rms_scale(tokens.astype(jnp.float32), g_attn).astype(jnp.bfloat16)
    query_low = rms_scale(
        jnp.dot(normed, w_query_down, preferred_element_type=jnp.float32), g_query
    ).astype(jnp.bfloat16)
    latent_new = rms_scale(
        jnp.dot(normed, w_latent_down, preferred_element_type=jnp.float32), g_latent
    ).astype(jnp.bfloat16)
    key_new = rotate(
        jnp.dot(normed, w_rope_key, preferred_element_type=jnp.float32), lengths
    ).astype(jnp.bfloat16)
    new_entry = jnp.concatenate([latent_new, key_new], axis=1)
    query_nope = jnp.dot(query_low, w_query, preferred_element_type=jnp.float32).astype(
        jnp.bfloat16
    )
    query_nope = query_nope.reshape(row_count, HEADS, NOPE)
    query_turn = jnp.dot(query_low, w_query_rope, preferred_element_type=jnp.float32).reshape(
        row_count, HEADS, ROPE
    )
    query_rope = rotate(query_turn, lengths).astype(jnp.bfloat16)
    query_latent = jnp.einsum(
        "bhn,chn->bhc",
        query_nope,
        w_key_up.reshape(KVLORA, HEADS, NOPE),
        preferred_element_type=jnp.float32,
    ).astype(jnp.bfloat16)
    scores = (
        jnp.einsum("shc,stc->sht", query_latent, latent_cache, preferred_element_type=jnp.float32)
        + jnp.einsum("shr,str->sht", query_rope, rope_cache, preferred_element_type=jnp.float32)
    ) * (NOPE + ROPE) ** (-0.5)
    live_mask = (
        jnp.arange(latent_cache.shape[1], dtype=jnp.int32)[None, None, :] < lengths[:, None, None]
    )
    row_max = jnp.max(jnp.where(live_mask, scores, masked_score), axis=2, keepdims=True)
    weights = jnp.where(live_mask, jnp.exp(scores - row_max), 0.0)
    weight_sum = jnp.sum(weights, axis=2)
    mixed_latent = jnp.einsum(
        "sht,stc->shc",
        weights.astype(jnp.bfloat16),
        latent_cache,
        preferred_element_type=jnp.float32,
    )
    latent_mix = (mixed_latent / weight_sum[:, :, None]).astype(jnp.bfloat16)
    value_heads = jnp.einsum(
        "shc,chv->shv",
        latent_mix,
        w_value_up.reshape(KVLORA, HEADS, VDIM),
        preferred_element_type=jnp.float32,
    ).astype(jnp.bfloat16)
    attn_out = jnp.dot(
        value_heads.reshape(row_count, HEADS * VDIM), w_out, preferred_element_type=jnp.float32
    )
    hidden_state = (tokens.astype(jnp.float32) + attn_out).astype(jnp.bfloat16)
    normed_ffn = rms_scale(hidden_state.astype(jnp.float32), g_ffn).astype(jnp.bfloat16)
    shared_gate = jnp.dot(normed_ffn, w_shared_gate, preferred_element_type=jnp.float32)
    shared_up = jnp.dot(normed_ffn, w_shared_up, preferred_element_type=jnp.float32)
    shared_hidden = (jax.nn.silu(shared_gate) * shared_up).astype(jnp.bfloat16)
    shared_out = jnp.dot(shared_hidden, w_shared_down, preferred_element_type=jnp.float32)
    meta = jnp.concatenate(
        [expert_ids.T.astype(jnp.float32).reshape(1, -1), route_weights.T.reshape(1, -1)], axis=1
    )
    base = hidden_state.astype(jnp.float32) + shared_out
    mixed_out = moe(normed_ffn, meta, base, w_expert_gate, w_expert_up, w_expert_down)
    return (mixed_out, new_entry)


def solution(mesh):
    in_specs = (
        P(("grp", "ep", "tp"), None),
        P(("grp", "ep", "tp"), None, None),
        P(("grp", "ep", "tp"), None, None),
        P(("grp", "ep", "tp")),
        P(("grp", "ep", "tp"), None),
        P(("grp", "ep", "tp"), None),
        P(),
        P(),
        P(),
        P(),
        P(),
        P(),
        P(),
        P(),
        P(),
        P(),
        P(),
        P(),
        P("ep", None, "tp"),
        P("ep", None, "tp"),
        P("ep", "tp", None),
        P(),
        P(),
        P(),
    )
    out_specs = (P(("grp", "ep", "tp"), None), P(("grp", "ep", "tp"), None))
    return jax.shard_map(local, mesh=mesh, in_specs=in_specs, out_specs=out_specs, check_vma=False)
```
